32 devices in a mesh: sp: 8 (over z, y), tp: 4 (over x, core).
Axes of the slice: x: 2, y: 2, z: 4, core: 2. Of those that a mesh axis runs over, the one named last changes fastest.
Arguments:
- resid_stream: bfloat16 [3072, 2048], P('sp'), may hold values from -6 to 6
- q_latent: bfloat16 [3072, 512], P('sp'), may hold values from -6 to 6
- kv_latent: bfloat16 [3072, 256], P('sp'), may hold values from -6 to 6
- rope_key: bfloat16 [3072, 64], P('sp'), may hold values from -6 to 6
- doc_ids: int32 [3072], P('sp'), may hold values from 0 to 3, as said below
- q_gain: float32 [512], replicated, may hold values from 1.5 to 64
- kv_gain: float32 [256], replicated, may hold values from 0.1 to 1.9
- w_query: bfloat16 [512, 3072], P(None, 'tp'), may hold values from -0.25 to 0.25
- w_key: bfloat16 [256, 2048], P(None, 'tp'), may hold values from -0.375 to 0.375
- w_value: bfloat16 [256, 2048], P(None, 'tp'), may hold values from -0.375 to 0.375
- w_out: bfloat16 [2048, 2048], replicated, may hold values from -0.5 to 0.5
- mix_gain: float32 [2048], replicated, may hold values from 0.1 to 1.9
- w_gate: bfloat16 [2048, 5632], P('sp', 'tp'), may hold values from -0.125 to 0.125
- w_up: bfloat16 [2048, 5632], P('sp', 'tp'), may hold values from -0.125 to 0.125
- w_down: bfloat16 [5632, 2048], P('tp', 'sp'), may hold values from -0.3125 to 0.3125
- out_gain: float32 [2048], replicated, may hold values from 0.1 to 1.9
Outputs:
- layer_out: bfloat16 [3072, 2048], P(('sp', 'tp'))
The draws below stay inside these ranges and needn't reach their ends.
Inputs may be any that keep to these rules, and one draw needn't show every extreme that they name: `doc_ids`: document numbers never fall along the sequence; every document has 1 to 2304 positions and one has exactly 2304.
All inputs are finite; a program needn't handle non-finite values.
Results may differ from the reference program's by a relative error of at most 0.02.
The reference program's roundings to bfloat16 on the way count: a program that leaves them out, or rounds other values in their place, can miss the bound.
Values may be sent and summed in bfloat16 or wider, within the bound.
A program may use at most 128 MiB of HBM per device.

```python
import math
import jax
import jax.numpy as jnp
from jax import lax

D = 2048
FF = 5632
HEADS = 16
NOPE = 128
RD = 64
VD = 128
QR = 512
KR = 256
TOK_DEV = 384
TOKENS = 3072
DOC_MOST = 2304
N_TP = 4


def draw_q_gain(key, part):
    return jnp.exp(jax.random.uniform(key, (QR,), jnp.float32, math.log(1.5), math.log(4.0)))


def draw_doc_ids(key, part):
    rest = TOKENS - DOC_MOST
    margin = max(1, rest // 6)
    key_slot = jax.random.fold_in(key, 11)
    key_first = jax.random.fold_in(key, 23)
    key_second = jax.random.fold_in(key, 37)
    big_slot = jax.random.randint(key_slot, (), 0, 4, dtype=jnp.int32)
    first_cut = jax.random.randint(key_first, (), margin, rest // 2, dtype=jnp.int32)
    second_cut = jax.random.randint(key_second, (), rest // 2 + margin, rest - margin + 1, dtype=jnp.int32)
    smaller = jnp.stack([first_cut, second_cut - first_cut, rest - second_cut]).astype(jnp.int32)
    slots = jnp.arange(4, dtype=jnp.int32)
    pick = slots - (slots > big_slot).astype(jnp.int32)
    pick = jnp.clip(pick, 0, 2)
    lengths = jnp.where(slots == big_slot, jnp.int32(DOC_MOST), jnp.take(smaller, pick))
    starts = jnp.cumsum(lengths).astype(jnp.int32)[:3]
    positions = jnp.arange(TOKENS, dtype=jnp.int32)
    return jnp.sum((positions[:, None] >= starts[None, :]).astype(jnp.int32), axis=1).astype(jnp.int32)


def shard_levels(stream_key, shape, split, low, largest):
    def one(axis_at, blocks):
        steps = jax.random.uniform(jax.random.fold_in(jax.random.fold_in(stream_key, 6), axis_at), (blocks,), jnp.float32, low / len(split), largest / len(split))
        return jnp.repeat(jnp.exp(steps), shape[axis_at] // blocks).reshape((-1,) + (1,) * (len(shape) - axis_at - 1))

    loudness = one(*split[0])
    for cut in split[1:]:
        loudness = loudness * one(*cut)
    return loudness


def normal_values(rng, dims, deviation, limit, shards=(), kind=jnp.bfloat16):
    values = jax.random.normal(rng, dims, jnp.float32) * deviation
    if len(shards) > 0:
        values = shard_levels(rng, dims, shards, -0.22, 0.18) * values
    return jnp.clip(values, min=-limit, max=limit).astype(kind)


def setup_inputs(seed: int = 0) -> dict:
    arg_keys = jax.random.split(jax.random.key(seed), 17)
    resid_stream = normal_values(arg_keys[0], (TOKENS, D), 1.0, 6.0, ((0, 8),))
    q_latent = normal_values(arg_keys[1], (TOKENS, QR), 1.0, 6.0, ((0, 8),))
    kv_latent = normal_values(arg_keys[2], (TOKENS, KR), 1.0, 6.0, ((0, 8),))
    rope_key = normal_values(arg_keys[3], (TOKENS, RD), 1.0, 6.0, ((0, 8),))
    doc_ids = draw_doc_ids(jax.random.fold_in(arg_keys[16], 71), 0)
    q_gain = draw_q_gain(jax.random.fold_in(arg_keys[16], 71), 0)
    kv_gain = jnp.clip(1.0 + 0.18 * jax.random.normal(arg_keys[6], (KR,), jnp.float32), 0.1, 1.9)
    w_query = normal_values(arg_keys[7], (QR, HEADS * (NOPE + RD)), QR ** -0.5, 0.25, ((1, 4),))
    w_key = normal_values(arg_keys[8], (KR, HEADS * NOPE), KR ** -0.5, 0.375, ((1, 4),))
    w_value = normal_values(arg_keys[9], (KR, HEADS * VD), KR ** -0.5, 0.375, ((1, 4),))
    w_out = normal_values(arg_keys[10], (HEADS * VD, D), (HEADS * VD // 16) ** -0.5, 0.5)
    mix_gain = jnp.clip(1.0 + 0.18 * jax.random.normal(arg_keys[11], (D,), jnp.float32), 0.1, 1.9)
    w_gate = normal_values(arg_keys[12], (D, FF), D ** -0.5, 0.125, ((0, 8), (1, 4)))
    w_up = normal_values(arg_keys[13], (D, FF), D ** -0.5, 0.125, ((0, 8), (1, 4)))
    w_down = normal_values(arg_keys[14], (FF, D), (FF // 16) ** -0.5, 0.3125, ((0, 4), (1, 8)))
    out_gain = jnp.clip(1.0 + 0.18 * jax.random.normal(arg_keys[15], (D,), jnp.float32), 0.1, 1.9)
    return dict(resid_stream=resid_stream, q_latent=q_latent, kv_latent=kv_latent, rope_key=rope_key, doc_ids=doc_ids, q_gain=q_gain, kv_gain=kv_gain, w_query=w_query, w_key=w_key, w_value=w_value, w_out=w_out, mix_gain=mix_gain, w_gate=w_gate, w_up=w_up, w_down=w_down, out_gain=out_gain)


eps_norm = 1e-05
rope_theta = 10000.0
resid_alpha = 8.0 ** 0.25

def rope_angles(positions):
    frequency = rope_theta ** (-jnp.arange(0, RD, 2, dtype=jnp.float32) / RD)
    angles = positions.astype(jnp.float32)[:, None] * frequency[None, :]
    return (jnp.cos(angles), jnp.sin(angles))

def rotate(values, cos_table, sin_table):
    half_width = values.shape[-1] // 2
    first_half = values[..., :half_width]
    second_half = values[..., half_width:]
    return jnp.concatenate([first_half * cos_table - second_half * sin_table, second_half * cos_table + first_half * sin_table], axis=-1)

def rms_scaled(latent, scaling):
    widened = latent.astype(jnp.float32)
    inverse = lax.rsqrt(lax.optimization_barrier(jnp.mean(widened * widened, axis=-1, keepdims=True)) + eps_norm)
    return (widened * inverse * scaling).astype(jnp.bfloat16)

def layer_scaled(stream, scaling):
    centre = stream - lax.optimization_barrier(jnp.mean(stream, axis=-1, keepdims=True))
    spread = lax.optimization_barrier(jnp.mean(centre * centre, axis=-1, keepdims=True))
    return centre * lax.rsqrt(spread + eps_norm) * scaling

def widen(packed):
    return lax.optimization_barrier(packed).astype(jnp.float32)

def reference(resid_stream, q_latent, kv_latent, rope_key, doc_ids, q_gain, kv_gain, w_query, w_key, w_value, w_out, mix_gain, w_gate, w_up, w_down, out_gain):
    positions = jnp.arange(TOKENS, dtype=jnp.int32)
    cos_table, sin_table = rope_angles(positions)
    q_normed = rms_scaled(q_latent, q_gain)
    queries = jnp.dot(q_normed, w_query, preferred_element_type=jnp.float32).reshape(TOKENS, HEADS, NOPE + RD)
    queries = jnp.concatenate([queries[:, :, :NOPE], rotate(queries[:, :, NOPE:], cos_table[:, None, :], sin_table[:, None, :])], axis=-1).astype(jnp.bfloat16)
    kv_normed = rms_scaled(kv_latent, kv_gain)
    key_nope = jnp.dot(kv_normed, w_key, preferred_element_type=jnp.float32).astype(jnp.bfloat16).reshape(TOKENS, HEADS, NOPE)
    values = jnp.dot(kv_normed, w_value, preferred_element_type=jnp.float32).astype(jnp.bfloat16).reshape(TOKENS, HEADS, VD)
    key_rot = rotate(rope_key.astype(jnp.float32), cos_table, sin_table).astype(jnp.bfloat16)
    score_scale = (NOPE + RD) ** (-0.5)
    key_wide = widen(key_nope)
    rot_wide = widen(key_rot)
    value_wide = widen(values)

    def one_block(block_index):
        first_row = (block_index * TOK_DEV).astype(jnp.int32)
        query_block = widen(lax.dynamic_slice_in_dim(queries, first_row, TOK_DEV, 0))
        doc_block = lax.dynamic_slice_in_dim(doc_ids, first_row, TOK_DEV, 0)
        scores = jnp.einsum('qhd,khd->hqk', query_block[:, :, :NOPE], key_wide)
        scores = (scores + jnp.einsum('qhd,kd->hqk', query_block[:, :, NOPE:], rot_wide)) * score_scale
        same_doc = (doc_block[:, None] == doc_ids[None, :])[None]
        masked = jnp.where(same_doc, scores, -1e+30)
        row_top = lax.optimization_barrier(jnp.max(masked, axis=-1, keepdims=True))
        weights = jnp.where(same_doc, jnp.exp(masked - row_top), 0.0)
        denom_sum = lax.optimization_barrier(jnp.sum(weights, axis=-1))
        weighted = jnp.einsum('hqk,khd->qhd', widen(weights.astype(jnp.bfloat16)), value_wide)
        return (weighted / jnp.transpose(denom_sum)[:, :, None]).astype(jnp.bfloat16)
    block_out = lax.map(one_block, jnp.arange(TOKENS // TOK_DEV, dtype=jnp.int32))
    attended = block_out.reshape(TOKENS, HEADS * VD)
    mixer_out = jnp.dot(attended, w_out, preferred_element_type=jnp.float32)
    normed_mid = layer_scaled(resid_alpha * resid_stream.astype(jnp.float32) + mixer_out, mix_gain).astype(jnp.bfloat16)
    gate_pre = jnp.dot(normed_mid, w_gate, preferred_element_type=jnp.float32)
    up_pre = jnp.dot(normed_mid, w_up, preferred_element_type=jnp.float32)
    hidden = (jax.nn.silu(gate_pre) * up_pre).astype(jnp.bfloat16)
    group_width = FF // N_TP
    ffn_sum = jnp.zeros((TOKENS, D), jnp.float32)
    for group_index in range(N_TP):
        partial_sum = jnp.dot(hidden[:, group_index * group_width:(group_index + 1) * group_width], w_down[group_index * group_width:(group_index + 1) * group_width, :], preferred_element_type=jnp.float32)
        ffn_sum = ffn_sum + widen(partial_sum.astype(jnp.bfloat16))
    layer_out = layer_scaled(resid_alpha * normed_mid.astype(jnp.float32) + 0.5 * ffn_sum, out_gain).astype(jnp.bfloat16)
    return layer_out
```

```python
import jax
import jax.numpy as jnp
from jax import lax
from jax.sharding import PartitionSpec as P

NOPE = 128
RD = 64
VD = 128


eps_norm = 1e-05
rope_theta = 10000.0
resid_alpha = 8.0**0.25
key_span = 2048


def rope_angles(positions):
    frequency = rope_theta ** (-jnp.arange(0, RD, 2, dtype=jnp.float32) / RD)
    angles = positions.astype(jnp.float32)[:, None] * frequency[None, :]
    return (jnp.cos(angles), jnp.sin(angles))


def rotate(values, cos_table, sin_table):
    half_width = values.shape[-1] // 2
    first_half = values[..., :half_width]
    second_half = values[..., half_width:]
    return jnp.concatenate(
        [
            first_half * cos_table - second_half * sin_table,
            second_half * cos_table + first_half * sin_table,
        ],
        axis=-1,
    )


def rms_scaled(latent, scaling):
    widened = latent.astype(jnp.float32)
    inverse = lax.rsqrt(jnp.mean(widened * widened, axis=-1, keepdims=True) + eps_norm)
    return (widened * inverse * scaling).astype(jnp.bfloat16)


def layer_scaled(stream, scaling):
    centre = stream - jnp.mean(stream, axis=-1, keepdims=True)
    spread = jnp.mean(centre * centre, axis=-1, keepdims=True)
    return centre * lax.rsqrt(spread + eps_norm) * scaling


def fold_in_blocks(carried, piece_part, attend_fn):
    piece_rows = piece_part[0].shape[0]
    if piece_rows > key_span and piece_rows % key_span == 0:

        def one_block(inner, block_index):
            sliced = tuple(
                (
                    lax.dynamic_slice_in_dim(
                        member, (block_index * key_span).astype(jnp.int32), key_span, 0
                    )
                    for member in piece_part
                )
            )
            return (attend_fn(inner, sliced), None)

        outcome = lax.scan(one_block, carried, jnp.arange(piece_rows // key_span, dtype=jnp.int32))
        return outcome[0]
    return attend_fn(carried, piece_part)


def ring_gather(block):
    count = lax.axis_size("sp")
    ring = list(range(0, count, 2)) + list(range(1, count, 2))[::-1]
    place = jnp.array([ring.index(i) for i in range(count)], jnp.int32)[lax.axis_index("sp")]
    ring_of = jnp.array(ring, jnp.int32)
    right = [(ring[i], ring[(i + 1) % count]) for i in range(count)]
    left = [(b, a) for a, b in right]
    pieces = [(lax.axis_index("sp"), block)]
    ahead, behind = block, block
    for step in range(1, count // 2):
        ahead = lax.ppermute(ahead, "sp", right)
        behind = lax.ppermute(behind, "sp", left)
        pieces.append((ring_of[(place - step) % count], ahead))
        pieces.append((ring_of[(place + step) % count], behind))
    half = block.shape[0] // 2
    ahead = lax.ppermute(ahead[:half], "sp", right)
    behind = lax.ppermute(behind[half:], "sp", left)
    pieces.append((ring_of[(place + count // 2) % count], jnp.concatenate([ahead, behind])))
    return pieces


def body(
    resid_stream,
    q_latent,
    kv_latent,
    rope_key,
    doc_ids,
    q_gain,
    kv_gain,
    w_query,
    w_key,
    w_value,
    w_out,
    mix_gain,
    w_gate,
    w_up,
    w_down,
    out_gain,
):
    tok_rows = q_latent.shape[0]
    head_count = w_key.shape[1] // NOPE
    tp_count = lax.axis_size("tp")
    part_rows = tok_rows // tp_count
    tp_index = lax.axis_index("tp")
    gate_up = ring_gather(jnp.concatenate([w_gate, w_up], axis=1))
    down = ring_gather(w_down)
    positions = lax.axis_index("sp") * tok_rows + jnp.arange(tok_rows, dtype=jnp.int32)
    cos_table, sin_table = rope_angles(positions)
    q_normed = rms_scaled(q_latent, q_gain)
    queries = jnp.dot(q_normed, w_query, preferred_element_type=jnp.float32).reshape(
        tok_rows, head_count, NOPE + RD
    )
    query_nope = queries[:, :, :NOPE].astype(jnp.bfloat16)
    query_rope = rotate(queries[:, :, NOPE:], cos_table[:, None, :], sin_table[:, None, :]).astype(
        jnp.bfloat16
    )
    kv_normed = rms_scaled(kv_latent, kv_gain)
    key_rot = rotate(rope_key.astype(jnp.float32), cos_table, sin_table).astype(jnp.bfloat16)
    score_scale = (NOPE + RD) ** (-0.5)

    def attend_rows(carried, piece_part):
        row_top, denom_sum, accum_out = carried
        key_piece, value_piece, rot_piece, doc_piece = piece_part
        piece_rows = key_piece.shape[0]
        keys_heads = key_piece.reshape(piece_rows, head_count, NOPE)
        values_heads = value_piece.reshape(piece_rows, head_count, VD)
        scores = jnp.einsum(
            "qhd,khd->hqk", query_nope, keys_heads, preferred_element_type=jnp.float32
        )
        scores = (
            scores
            + jnp.einsum("qhd,kd->hqk", query_rope, rot_piece, preferred_element_type=jnp.float32)
        ) * score_scale
        same_doc = (doc_ids[:, None] == doc_piece[None, :])[None]
        masked = jnp.where(same_doc, scores, -1e30)
        new_top = jnp.maximum(row_top, jnp.max(masked, axis=-1))
        weights = jnp.where(same_doc, jnp.exp(masked - new_top[:, :, None]), 0.0)
        factor = jnp.exp(row_top - new_top)
        denom_sum = denom_sum * factor + jnp.sum(weights, axis=-1)
        update = jnp.einsum(
            "hqk,khd->qhd",
            weights.astype(jnp.bfloat16),
            values_heads,
            preferred_element_type=jnp.float32,
        )
        accum_out = accum_out * jnp.transpose(factor)[:, :, None] + update
        return (new_top, denom_sum, accum_out)

    initial = (
        jnp.full((head_count, tok_rows), -1e30, jnp.float32),
        jnp.zeros((head_count, tok_rows), jnp.float32),
        jnp.zeros((tok_rows, head_count, VD), jnp.float32),
    )

    def project_rows(carried, piece_part):
        latent_piece, rot_piece, doc_piece = piece_part
        key_piece = jnp.dot(latent_piece, w_key, preferred_element_type=jnp.float32).astype(
            jnp.bfloat16
        )
        value_piece = jnp.dot(latent_piece, w_value, preferred_element_type=jnp.float32).astype(
            jnp.bfloat16
        )
        return attend_rows(carried, (key_piece, value_piece, rot_piece, doc_piece))

    doc_lanes = jnp.broadcast_to(doc_ids.astype(jnp.bfloat16)[:, None], (tok_rows, RD))
    packed = jnp.concatenate([kv_normed, key_rot, doc_lanes], axis=1)
    packed_all = lax.all_gather(packed, "sp", axis=0, tiled=True)
    kv_rank = kv_latent.shape[1]
    carried_out = fold_in_blocks(
        initial,
        (
            packed_all[:, :kv_rank],
            packed_all[:, kv_rank : kv_rank + RD],
            packed_all[:, kv_rank + RD].astype(jnp.int32),
        ),
        project_rows,
    )
    denom_sum = carried_out[1]
    attended = (
        (carried_out[2] / jnp.transpose(denom_sum)[:, :, None])
        .astype(jnp.bfloat16)
        .reshape(tok_rows, head_count * VD)
    )
    heads_rows = lax.all_to_all(attended, "tp", split_axis=0, concat_axis=1, tiled=True)
    mixer_out = jnp.dot(heads_rows, w_out, preferred_element_type=jnp.float32)
    own_resid = lax.dynamic_slice_in_dim(resid_stream, tp_index * part_rows, part_rows, 0)
    own_normed = layer_scaled(
        resid_alpha * own_resid.astype(jnp.float32) + mixer_out, mix_gain
    ).astype(jnp.bfloat16)
    normed_rows = lax.all_gather(own_normed, "tp", axis=0, tiled=True)
    gate_sum = None
    for owner, piece in gate_up:
        rows = lax.dynamic_slice_in_dim(normed_rows, owner * piece.shape[0], piece.shape[0], 1)
        term = jnp.dot(rows, piece, preferred_element_type=jnp.float32)
        gate_sum = term if gate_sum is None else gate_sum + term
    width = w_gate.shape[1]
    hidden = (jax.nn.silu(gate_sum[:, :width]) * gate_sum[:, width:]).astype(jnp.bfloat16)
    partial = jnp.zeros((tok_rows, resid_stream.shape[1]), jnp.bfloat16)
    for owner, piece in down:
        term = jnp.dot(hidden, piece, preferred_element_type=jnp.float32).astype(jnp.bfloat16)
        partial = lax.dynamic_update_slice_in_dim(partial, term, owner * piece.shape[1], 1)
    swapped = lax.all_to_all(
        partial.reshape(tp_count, part_rows, -1), "tp", split_axis=0, concat_axis=0, tiled=True
    )
    ffn_sum = jnp.sum(swapped.astype(jnp.float32), axis=0)
    layer_out = layer_scaled(
        resid_alpha * own_normed.astype(jnp.float32) + 0.5 * ffn_sum, out_gain
    ).astype(jnp.bfloat16)
    return layer_out


def solution(mesh):
    in_specs = (
        P("sp", None),
        P("sp", None),
        P("sp", None),
        P("sp", None),
        P("sp"),
        P(),
        P(),
        P(None, "tp"),
        P(None, "tp"),
        P(None, "tp"),
        P(),
        P(),
        P("sp", "tp"),
        P("sp", "tp"),
        P("tp", "sp"),
        P(),
    )
    out_specs = P(("sp", "tp"), None)
    return jax.shard_map(body, mesh=mesh, in_specs=in_specs, out_specs=out_specs, check_vma=False)
```

```python
import jax
import jax.numpy as jnp
from jax import lax
from jax.sharding import PartitionSpec as P

NOPE = 128
RD = 64
VD = 128


eps_norm = 1e-05
rope_theta = 10000.0
resid_alpha = 8.0**0.25
key_span = 2048


def rope_angles(positions):
    frequency = rope_theta ** (-jnp.arange(0, RD, 2, dtype=jnp.float32) / RD)
    angles = positions.astype(jnp.float32)[:, None] * frequency[None, :]
    return (jnp.cos(angles), jnp.sin(angles))


def rotate(values, cos_table, sin_table):
    half_width = values.shape[-1] // 2
    first_half = values[..., :half_width]
    second_half = values[..., half_width:]
    return jnp.concatenate(
        [
            first_half * cos_table - second_half * sin_table,
            second_half * cos_table + first_half * sin_table,
        ],
        axis=-1,
    )


def rms_scaled(latent, scaling):
    widened = latent.astype(jnp.float32)
    inverse = lax.rsqrt(jnp.mean(widened * widened, axis=-1, keepdims=True) + eps_norm)
    return (widened * inverse * scaling).astype(jnp.bfloat16)


def layer_scaled(stream, scaling):
    centre = stream - jnp.mean(stream, axis=-1, keepdims=True)
    spread = jnp.mean(centre * centre, axis=-1, keepdims=True)
    return centre * lax.rsqrt(spread + eps_norm) * scaling


def fold_in_blocks(carried, piece_part, attend_fn):
    piece_rows = piece_part[0].shape[0]
    if piece_rows > key_span and piece_rows % key_span == 0:

        def one_block(inner, block_index):
            sliced = tuple(
                (
                    lax.dynamic_slice_in_dim(
                        member, (block_index * key_span).astype(jnp.int32), key_span, 0
                    )
                    for member in piece_part
                )
            )
            return (attend_fn(inner, sliced), None)

        outcome = lax.scan(one_block, carried, jnp.arange(piece_rows // key_span, dtype=jnp.int32))
        return outcome[0]
    return attend_fn(carried, piece_part)


class Ring:
    def __init__(self, blocks):
        self.count = lax.axis_size("sp")
        ring = list(range(0, self.count, 2)) + list(range(1, self.count, 2))[::-1]
        places = [ring.index(i) for i in range(self.count)]
        self.place = jnp.array(places, jnp.int32)[lax.axis_index("sp")]
        self.ring_of = jnp.array(ring, jnp.int32)
        self.right = [(ring[i], ring[(i + 1) % self.count]) for i in range(self.count)]
        self.left = [(after, before) for before, after in self.right]
        self.pieces = [[(lax.axis_index("sp"), block)] for block in blocks]
        self.flying = [(block, block) for block in blocks]
        self.step = 0

    def owner(self, distance):
        return self.ring_of[(self.place + distance) % self.count]

    def hop(self):
        self.step += 1
        self.send()

    def send(self):
        if self.step < self.count // 2:
            self.flying = [
                (lax.ppermute(one, "sp", self.right), lax.ppermute(two, "sp", self.left))
                for one, two in self.flying
            ]
        elif self.step == self.count // 2:
            self.flying = [
                (
                    lax.ppermute(one[: one.shape[0] // 2], "sp", self.right),
                    lax.ppermute(two[two.shape[0] // 2 :], "sp", self.left),
                )
                for one, two in self.flying
            ]

    def land(self, *values):
        if self.step <= self.count // 2:
            if values:
                values, self.flying = lax.optimization_barrier((values, self.flying))
            for pieces, (one, two) in zip(self.pieces, self.flying):
                if self.step < self.count // 2:
                    pieces.append((self.owner(-self.step), one))
                    pieces.append((self.owner(self.step), two))
                else:
                    pieces.append((self.owner(self.step), jnp.concatenate([one, two])))
        return values


def body(
    resid_stream,
    q_latent,
    kv_latent,
    rope_key,
    doc_ids,
    q_gain,
    kv_gain,
    w_query,
    w_key,
    w_value,
    w_out,
    mix_gain,
    w_gate,
    w_up,
    w_down,
    out_gain,
):
    tok_rows = q_latent.shape[0]
    head_count = w_key.shape[1] // NOPE
    tp_count = lax.axis_size("tp")
    part_rows = tok_rows // tp_count
    tp_index = lax.axis_index("tp")
    ring = Ring([jnp.concatenate([w_gate, w_up], axis=1), w_down])
    ring.hop()
    positions = lax.axis_index("sp") * tok_rows + jnp.arange(tok_rows, dtype=jnp.int32)
    cos_table, sin_table = rope_angles(positions)
    q_normed = rms_scaled(q_latent, q_gain)
    queries = jnp.dot(q_normed, w_query, preferred_element_type=jnp.float32).reshape(
        tok_rows, head_count, NOPE + RD
    )
    query_nope = queries[:, :, :NOPE].astype(jnp.bfloat16)
    query_rope = rotate(queries[:, :, NOPE:], cos_table[:, None, :], sin_table[:, None, :]).astype(
        jnp.bfloat16
    )
    kv_normed = rms_scaled(kv_latent, kv_gain)
    key_rot = rotate(rope_key.astype(jnp.float32), cos_table, sin_table).astype(jnp.bfloat16)
    score_scale = (NOPE + RD) ** (-0.5)

    def attend_rows(carried, piece_part, between=lambda value: value):
        row_top, denom_sum, accum_out = carried
        key_piece, value_piece, rot_piece, doc_piece = piece_part
        piece_rows = key_piece.shape[0]
        keys_heads = key_piece.reshape(piece_rows, head_count, NOPE)
        values_heads = value_piece.reshape(piece_rows, head_count, VD)
        scores = jnp.einsum(
            "qhd,khd->hqk", query_nope, keys_heads, preferred_element_type=jnp.float32
        )
        scores = (
            scores
            + jnp.einsum("qhd,kd->hqk", query_rope, rot_piece, preferred_element_type=jnp.float32)
        ) * score_scale
        same_doc = (doc_ids[:, None] == doc_piece[None, :])[None]
        masked = jnp.where(same_doc, scores, -1e30)
        new_top = jnp.maximum(row_top, jnp.max(masked, axis=-1))
        weights = jnp.where(same_doc, jnp.exp(masked - new_top[:, :, None]), 0.0)
        factor = jnp.exp(row_top - new_top)
        denom_sum = denom_sum * factor + jnp.sum(weights, axis=-1)
        weights = between(weights.astype(jnp.bfloat16))
        update = jnp.einsum(
            "hqk,khd->qhd", weights, values_heads, preferred_element_type=jnp.float32
        )
        accum_out = accum_out * jnp.transpose(factor)[:, :, None] + update
        return (new_top, denom_sum, accum_out)

    initial = (
        jnp.full((head_count, tok_rows), -1e30, jnp.float32),
        jnp.zeros((head_count, tok_rows), jnp.float32),
        jnp.zeros((tok_rows, head_count, VD), jnp.float32),
    )

    def project_rows(carried, piece_part, between=lambda value: value):
        latent_piece, rot_piece, doc_piece = piece_part
        key_piece = jnp.dot(latent_piece, w_key, preferred_element_type=jnp.float32).astype(
            jnp.bfloat16
        )
        value_piece = jnp.dot(latent_piece, w_value, preferred_element_type=jnp.float32).astype(
            jnp.bfloat16
        )
        return attend_rows(carried, (key_piece, value_piece, rot_piece, doc_piece), between)

    def next_hop(value):
        (value,) = ring.land(value)
        ring.hop()
        return value

    doc_lanes = jnp.broadcast_to(doc_ids.astype(jnp.bfloat16)[:, None], (tok_rows, RD))
    packed = jnp.concatenate([kv_normed, key_rot, doc_lanes], axis=1)
    packed_all = lax.all_gather(packed, "sp", axis=0, tiled=True)
    packed_all = next_hop(packed_all)
    kv_rank = kv_latent.shape[1]
    gathered = (
        packed_all[:, :kv_rank],
        packed_all[:, kv_rank : kv_rank + RD],
        packed_all[:, kv_rank + RD].astype(jnp.int32),
    )
    if packed_all.shape[0] > key_span and packed_all.shape[0] % key_span == 0:
        carried_out = fold_in_blocks(initial, gathered, project_rows)
    else:
        carried_out = project_rows(initial, gathered, next_hop)
    denom_sum = carried_out[1]
    attended = (
        (carried_out[2] / jnp.transpose(denom_sum)[:, :, None])
        .astype(jnp.bfloat16)
        .reshape(tok_rows, head_count * VD)
    )
    heads_rows = lax.all_to_all(attended, "tp", split_axis=0, concat_axis=1, tiled=True)
    mixer_out = jnp.dot(heads_rows, w_out, preferred_element_type=jnp.float32)
    own_resid = lax.dynamic_slice_in_dim(resid_stream, tp_index * part_rows, part_rows, 0)
    own_normed = layer_scaled(
        resid_alpha * own_resid.astype(jnp.float32) + mixer_out, mix_gain
    ).astype(jnp.bfloat16)
    own_normed = next_hop(own_normed)
    normed_rows = lax.all_gather(own_normed, "tp", axis=0, tiled=True)
    ring.land()
    while ring.step < ring.count // 2:
        ring.hop()
        ring.land()
    gate_up, down = ring.pieces
    gate_sum = None
    for owner, piece in gate_up:
        rows = lax.dynamic_slice_in_dim(normed_rows, owner * piece.shape[0], piece.shape[0], 1)
        term = jnp.dot(rows, piece, preferred_element_type=jnp.float32)
        gate_sum = term if gate_sum is None else gate_sum + term
    width = w_gate.shape[1]
    hidden = (jax.nn.silu(gate_sum[:, :width]) * gate_sum[:, width:]).astype(jnp.bfloat16)
    ffn_sum = jnp.zeros((part_rows, resid_stream.shape[1]), jnp.float32)
    for group in (down[: len(down) // 2], down[len(down) // 2 :]):
        partial = jnp.concatenate(
            [
                jnp.dot(hidden, piece, preferred_element_type=jnp.float32).astype(jnp.bfloat16)
                for _, piece in group
            ],
            axis=1,
        )
        swapped = lax.all_to_all(
            partial.reshape(tp_count, part_rows, -1), "tp", split_axis=0, concat_axis=0, tiled=True
        )
        summed = jnp.sum(swapped.astype(jnp.float32), axis=0)
        columns = w_down.shape[1]
        for at, (owner, _) in enumerate(group):
            ffn_sum = lax.dynamic_update_slice_in_dim(
                ffn_sum, summed[:, at * columns : (at + 1) * columns], owner * columns, 1
            )
    layer_out = layer_scaled(
        resid_alpha * own_normed.astype(jnp.float32) + 0.5 * ffn_sum, out_gain
    ).astype(jnp.bfloat16)
    return layer_out


def solution(mesh):
    in_specs = (
        P("sp", None),
        P("sp", None),
        P("sp", None),
        P("sp", None),
        P("sp"),
        P(),
        P(),
        P(None, "tp"),
        P(None, "tp"),
        P(None, "tp"),
        P(),
        P(),
        P("sp", "tp"),
        P("sp", "tp"),
        P("tp", "sp"),
        P(),
    )
    out_specs = P(("sp", "tp"), None)
    return jax.shard_map(body, mesh=mesh, in_specs=in_specs, out_specs=out_specs, check_vma=False)
```

```python
import jax
import jax.numpy as jnp
from jax import lax
from jax.sharding import PartitionSpec as P

NOPE = 128
RD = 64
VD = 128


eps_norm = 1e-05
rope_theta = 10000.0
resid_alpha = 8.0**0.25
key_span = 2048


def rope_angles(positions):
    frequency = rope_theta ** (-jnp.arange(0, RD, 2, dtype=jnp.float32) / RD)
    angles = positions.astype(jnp.float32)[:, None] * frequency[None, :]
    return (jnp.cos(angles), jnp.sin(angles))


def rotate(values, cos_table, sin_table):
    half_width = values.shape[-1] // 2
    first_half = values[..., :half_width]
    second_half = values[..., half_width:]
    return jnp.concatenate(
        [
            first_half * cos_table - second_half * sin_table,
            second_half * cos_table + first_half * sin_table,
        ],
        axis=-1,
    )


def rms_scaled(latent, scaling):
    widened = latent.astype(jnp.float32)
    inverse = lax.rsqrt(jnp.mean(widened * widened, axis=-1, keepdims=True) + eps_norm)
    return (widened * inverse * scaling).astype(jnp.bfloat16)


def layer_scaled(stream, scaling):
    centre = stream - jnp.mean(stream, axis=-1, keepdims=True)
    spread = jnp.mean(centre * centre, axis=-1, keepdims=True)
    return centre * lax.rsqrt(spread + eps_norm) * scaling


def fold_in_blocks(carried, piece_part, attend_fn):
    piece_rows = piece_part[0].shape[0]
    if piece_rows > key_span and piece_rows % key_span == 0:

        def one_block(inner, block_index):
            sliced = tuple(
                (
                    lax.dynamic_slice_in_dim(
                        member, (block_index * key_span).astype(jnp.int32), key_span, 0
                    )
                    for member in piece_part
                )
            )
            return (attend_fn(inner, sliced), None)

        outcome = lax.scan(one_block, carried, jnp.arange(piece_rows // key_span, dtype=jnp.int32))
        return outcome[0]
    return attend_fn(carried, piece_part)


class Ring:
    def __init__(self, blocks):
        self.count = lax.axis_size("sp")
        ring = list(range(0, self.count, 2)) + list(range(1, self.count, 2))[::-1]
        places = [ring.index(i) for i in range(self.count)]
        self.place = jnp.array(places, jnp.int32)[lax.axis_index("sp")]
        self.ring_of = jnp.array(ring, jnp.int32)
        self.right = [(ring[i], ring[(i + 1) % self.count]) for i in range(self.count)]
        self.left = [(after, before) for before, after in self.right]
        self.pieces = [[(lax.axis_index("sp"), block)] for block in blocks]
        self.flying = [(block, block) for block in blocks]
        self.step = 0

    def owner(self, distance):
        return self.ring_of[(self.place + distance) % self.count]

    def hop(self):
        self.step += 1
        self.send()

    def send(self):
        if self.step < self.count // 2:
            self.flying = [
                (lax.ppermute(one, "sp", self.right), lax.ppermute(two, "sp", self.left))
                for one, two in self.flying
            ]
        elif self.step == self.count // 2:
            self.flying = [
                (
                    lax.ppermute(one[: one.shape[0] // 2], "sp", self.right),
                    lax.ppermute(two[two.shape[0] // 2 :], "sp", self.left),
                )
                for one, two in self.flying
            ]

    def land(self, *values):
        if self.step <= self.count // 2:
            if values:
                values, self.flying = lax.optimization_barrier((values, self.flying))
            for pieces, (one, two) in zip(self.pieces, self.flying):
                if self.step < self.count // 2:
                    pieces.append((self.owner(-self.step), one))
                    pieces.append((self.owner(self.step), two))
                else:
                    pieces.append((self.owner(self.step), jnp.concatenate([one, two])))
        return values


def body(
    resid_stream,
    q_latent,
    kv_latent,
    rope_key,
    doc_ids,
    q_gain,
    kv_gain,
    w_query,
    w_key,
    w_value,
    w_out,
    mix_gain,
    w_gate,
    w_up,
    w_down,
    out_gain,
):
    tok_rows = q_latent.shape[0]
    head_count = w_key.shape[1] // NOPE
    tp_count = lax.axis_size("tp")
    part_rows = tok_rows // tp_count
    tp_index = lax.axis_index("tp")
    gate_ring = Ring([jnp.concatenate([w_gate, w_up], axis=1)])
    down_ring = Ring([w_down])
    gate_ring.hop()
    positions = lax.axis_index("sp") * tok_rows + jnp.arange(tok_rows, dtype=jnp.int32)
    cos_table, sin_table = rope_angles(positions)
    q_normed = rms_scaled(q_latent, q_gain)
    queries = jnp.dot(q_normed, w_query, preferred_element_type=jnp.float32).reshape(
        tok_rows, head_count, NOPE + RD
    )
    query_nope = queries[:, :, :NOPE].astype(jnp.bfloat16)
    query_rope = rotate(queries[:, :, NOPE:], cos_table[:, None, :], sin_table[:, None, :]).astype(
        jnp.bfloat16
    )
    kv_normed = rms_scaled(kv_latent, kv_gain)
    key_rot = rotate(rope_key.astype(jnp.float32), cos_table, sin_table).astype(jnp.bfloat16)
    score_scale = (NOPE + RD) ** (-0.5)

    def attend_rows(carried, piece_part, between=lambda value: value):
        row_top, denom_sum, accum_out = carried
        key_piece, value_piece, rot_piece, doc_piece = piece_part
        piece_rows = key_piece.shape[0]
        keys_heads = key_piece.reshape(piece_rows, head_count, NOPE)
        values_heads = value_piece.reshape(piece_rows, head_count, VD)
        scores = jnp.einsum(
            "qhd,khd->hqk", query_nope, keys_heads, preferred_element_type=jnp.float32
        )
        scores = (
            scores
            + jnp.einsum("qhd,kd->hqk", query_rope, rot_piece, preferred_element_type=jnp.float32)
        ) * score_scale
        same_doc = (doc_ids[:, None] == doc_piece[None, :])[None]
        masked = jnp.where(same_doc, scores, -1e30)
        new_top = jnp.maximum(row_top, jnp.max(masked, axis=-1))
        weights = jnp.where(same_doc, jnp.exp(masked - new_top[:, :, None]), 0.0)
        factor = jnp.exp(row_top - new_top)
        denom_sum = denom_sum * factor + jnp.sum(weights, axis=-1)
        weights = between(weights.astype(jnp.bfloat16))
        update = jnp.einsum(
            "hqk,khd->qhd", weights, values_heads, preferred_element_type=jnp.float32
        )
        accum_out = accum_out * jnp.transpose(factor)[:, :, None] + update
        return (new_top, denom_sum, accum_out)

    initial = (
        jnp.full((head_count, tok_rows), -1e30, jnp.float32),
        jnp.zeros((head_count, tok_rows), jnp.float32),
        jnp.zeros((tok_rows, head_count, VD), jnp.float32),
    )

    def project_rows(carried, piece_part, between=lambda value: value):
        latent_piece, rot_piece, doc_piece = piece_part
        key_piece = jnp.dot(latent_piece, w_key, preferred_element_type=jnp.float32).astype(
            jnp.bfloat16
        )
        value_piece = jnp.dot(latent_piece, w_value, preferred_element_type=jnp.float32).astype(
            jnp.bfloat16
        )
        return attend_rows(carried, (key_piece, value_piece, rot_piece, doc_piece), between)

    def next_hop(value):
        (value,) = gate_ring.land(value)
        gate_ring.hop()
        return value

    doc_lanes = jnp.broadcast_to(doc_ids.astype(jnp.bfloat16)[:, None], (tok_rows, RD))
    packed = jnp.concatenate([kv_normed, key_rot, doc_lanes], axis=1)
    packed_part = lax.dynamic_slice_in_dim(packed, tp_index * part_rows, part_rows, 0)
    packed_all = lax.all_gather(packed_part, ("sp", "tp"), axis=0, tiled=True)
    packed_all = next_hop(packed_all)
    kv_rank = kv_latent.shape[1]
    gathered = (
        packed_all[:, :kv_rank],
        packed_all[:, kv_rank : kv_rank + RD],
        packed_all[:, kv_rank + RD].astype(jnp.int32),
    )
    if packed_all.shape[0] > key_span and packed_all.shape[0] % key_span == 0:
        carried_out = fold_in_blocks(initial, gathered, project_rows)
    else:
        carried_out = project_rows(initial, gathered, next_hop)
    denom_sum = carried_out[1]
    attended = (
        (carried_out[2] / jnp.transpose(denom_sum)[:, :, None])
        .astype(jnp.bfloat16)
        .reshape(tok_rows, head_count * VD)
    )
    heads_rows = lax.all_to_all(attended, "tp", split_axis=0, concat_axis=1, tiled=True)
    mixer_out = jnp.dot(heads_rows, w_out, preferred_element_type=jnp.float32)
    own_resid = lax.dynamic_slice_in_dim(resid_stream, tp_index * part_rows, part_rows, 0)
    own_normed = layer_scaled(
        resid_alpha * own_resid.astype(jnp.float32) + mixer_out, mix_gain
    ).astype(jnp.bfloat16)
    (own_normed,) = gate_ring.land(own_normed)
    down_ring.hop()
    gate_ring.hop()
    normed_rows = lax.all_gather(own_normed, "tp", axis=0, tiled=True)
    (normed_rows,) = down_ring.land(normed_rows)
    down_ring.hop()
    gate_ring.land()
    while gate_ring.step < gate_ring.count // 2:
        gate_ring.hop()
        gate_ring.land()
    gate_sum = None
    for owner, piece in gate_ring.pieces[0]:
        rows = lax.dynamic_slice_in_dim(normed_rows, owner * piece.shape[0], piece.shape[0], 1)
        term = jnp.dot(rows, piece, preferred_element_type=jnp.float32)
        gate_sum = term if gate_sum is None else gate_sum + term
    width = w_gate.shape[1]
    hidden = (jax.nn.silu(gate_sum[:, :width]) * gate_sum[:, width:]).astype(jnp.bfloat16)
    (hidden,) = down_ring.land(hidden)
    while down_ring.step < down_ring.count // 2:
        down_ring.hop()
        down_ring.land()
    down = down_ring.pieces[0]
    ffn_sum = jnp.zeros((part_rows, resid_stream.shape[1]), jnp.float32)
    for part, group in enumerate((down[: len(down) // 2], down[len(down) // 2 :])):
        pieces = [piece for _, piece in group]
        if part == 0:
            pieces = [jnp.concatenate(pieces, axis=1)]
        terms = [
            jnp.dot(hidden, piece, preferred_element_type=jnp.float32).astype(jnp.bfloat16)
            for piece in pieces
        ]
        partial = jnp.concatenate(terms, axis=1)
        swapped = lax.all_to_all(
            partial.reshape(tp_count, part_rows, -1), "tp", split_axis=0, concat_axis=0, tiled=True
        )
        summed = jnp.sum(swapped.astype(jnp.float32), axis=0)
        columns = w_down.shape[1]
        for at, (owner, _) in enumerate(group):
            ffn_sum = lax.dynamic_update_slice_in_dim(
                ffn_sum, summed[:, at * columns : (at + 1) * columns], owner * columns, 1
            )
    layer_out = layer_scaled(
        resid_alpha * own_normed.astype(jnp.float32) + 0.5 * ffn_sum, out_gain
    ).astype(jnp.bfloat16)
    return layer_out


def solution(mesh):
    in_specs = (
        P("sp", None),
        P("sp", None),
        P("sp", None),
        P("sp", None),
        P("sp"),
        P(),
        P(),
        P(None, "tp"),
        P(None, "tp"),
        P(None, "tp"),
        P(),
        P(),
        P("sp", "tp"),
        P("sp", "tp"),
        P("tp", "sp"),
        P(),
    )
    out_specs = P(("sp", "tp"), None)
    return jax.shard_map(body, mesh=mesh, in_specs=in_specs, out_specs=out_specs, check_vma=False)
```
